128 devices in a mesh: fs: 16 (over z, x), tp: 8 (over y, core).
Axes of the slice: x: 4, y: 4, z: 4, core: 2. Of those that a mesh axis runs over, the one named last changes fastest.
Arguments:
- later_rows: bfloat16 [14336, 2048], P(('fs', 'tp')), may hold values from -6 to 6
- earlier_rows: bfloat16 [14336, 2048], P(('fs', 'tp')), may hold values from -6 to 6
- cotangent: bfloat16 [14336, 2048], P(('fs', 'tp')), may hold values from -1 to 1
- gate_weight: bfloat16 [2048, 5632], P('fs', 'tp'), may hold values from -0.125 to 0.125
- up_weight: bfloat16 [2048, 5632], P('fs', 'tp'), may hold values from -0.125 to 0.125
- down_weight: bfloat16 [2048, 5632], P('fs', 'tp'), may hold values from -0.078125 to 0.078125
- gate_grad_sum: float32 [2048, 5632], P('fs', 'tp'), may hold values from -12 to 12
- up_grad_sum: float32 [2048, 5632], P('fs', 'tp'), may hold values from -12 to 12
- down_grad_sum: float32 [2048, 5632], P('fs', 'tp'), may hold values from -12 to 12
Outputs:
- later_out: bfloat16 [14336, 2048], P(('fs', 'tp'))
- input_grad: bfloat16 [14336, 2048], P(('fs', 'tp'))
- gate_grad_new: float32 [2048, 5632], P('fs', 'tp')
- up_grad_new: float32 [2048, 5632], P('fs', 'tp')
- down_grad_new: float32 [2048, 5632], P('fs', 'tp')
The draws below stay inside these ranges and needn't reach their ends.
All inputs are finite; a program needn't handle non-finite values.
Results may differ from the reference program's by a relative error of at most 0.014.
Values may be sent and summed in bfloat16 or wider, within the bound.
No kernel may reach another device: no remote copies, remote signals or barrier semaphores. Data moves between devices by JAX's collectives and lax.ppermute only.
A program may use at most 128 MiB of HBM per device.

```python
import jax
import jax.numpy as jnp
from jax import lax

D = 2048
FF = 5632
TOKENS = 14336
N_TP = 8


def strengthened(values, stream_key, source, target, parts, factor):
    def block_of(position):
        return (jnp.arange(values.shape[position]) // (values.shape[position] // parts)).reshape((-1,) + (1,) * (values.ndim - 1 - position))

    first = jax.random.permutation(stream_key, parts)[block_of(target)]
    other_side = (block_of(target) + parts // 2) % parts
    return jnp.where((block_of(source) == first) | (block_of(source) == other_side), factor * values, values)


def block_scale(rng, shape, split, smallest, high):
    gain = 1.0
    for axis_at, shards_of in split:
        heights = jax.random.uniform(jax.random.fold_in(jax.random.fold_in(rng, 6), axis_at), (shards_of,), jnp.float32, smallest / len(split), high / len(split))
        gain = gain * jnp.repeat(jnp.exp(heights), shape[axis_at] // shards_of).reshape((-1,) + (1,) * (len(shape) - 1 - axis_at))
    return gain


def scatter_about(stream_key, shape, spread, limit, cuts=(), kind=jnp.bfloat16):
    drawn = jax.random.normal(stream_key, shape, jnp.float32) * spread
    if len(cuts) > 0:
        drawn = block_scale(stream_key, shape, cuts, -0.22, 0.18) * drawn
    return jnp.clip(drawn, min=-limit, max=limit).astype(kind)


def noise_with(rng, dims, spread, most, shards, heavy, held_as=jnp.bfloat16):
    drawn = spread * jax.random.normal(rng, dims, jnp.float32)
    if shards:
        drawn = drawn * block_scale(rng, dims, shards, -0.22, 0.18)
    return jnp.clip(strengthened(drawn, jax.random.fold_in(rng, 3), *heavy), -most, most).astype(held_as)


def setup_inputs(seed: int = 0) -> dict:
    streams_of = jax.random.split(jax.random.key(seed), 10)
    return {
        "later_rows": scatter_about(streams_of[0], (TOKENS, D), 1.0, 6.0, ((0, 128),)),
        "earlier_rows": scatter_about(streams_of[1], (TOKENS, D), 1.0, 6.0, ((0, 128),)),
        "cotangent": noise_with(streams_of[2], (TOKENS, D), 0.1, 1.0, ((0, 128),), (0, 1, 128, 5.5)),
        "gate_weight": scatter_about(streams_of[3], (D, FF), D ** -0.5, 0.125, ((0, 16), (1, 8))),
        "up_weight": scatter_about(streams_of[4], (D, FF), D ** -0.5, 0.125, ((0, 16), (1, 8))),
        "down_weight": scatter_about(streams_of[5], (D, FF), FF ** -0.5, 0.078125, ((0, 16), (1, 8))),
        "gate_grad_sum": scatter_about(streams_of[6], (D, FF), 2.0, 12.0, ((0, 16), (1, 8)), jnp.float32),
        "up_grad_sum": scatter_about(streams_of[7], (D, FF), 2.0, 12.0, ((0, 16), (1, 8)), jnp.float32),
        "down_grad_sum": scatter_about(streams_of[8], (D, FF), 2.0, 12.0, ((0, 16), (1, 8)), jnp.float32),
    }


def silu_parts(gate):
    sigma = jax.nn.sigmoid(gate)
    return gate * sigma, sigma * (1.0 + gate * (1.0 - sigma))


def by_columns(left, right):
    return lax.dot_general(left, right, (((1,), (1,)), ((), ())), preferred_element_type=jnp.float32)


def by_rows(left, right):
    return lax.dot_general(left, right, (((0,), (0,)), ((), ())), preferred_element_type=jnp.float32)


def reference(later_rows, earlier_rows, cotangent, gate_weight, up_weight, down_weight, gate_grad_sum, up_grad_sum, down_grad_sum):
    width = FF // N_TP
    later_gate = jnp.dot(later_rows, gate_weight, preferred_element_type=jnp.float32)
    later_up = jnp.dot(later_rows, up_weight, preferred_element_type=jnp.float32)
    later_hidden = (jax.nn.silu(later_gate) * later_up).astype(jnp.bfloat16)
    total = jnp.zeros((later_rows.shape[0], D), jnp.float32)
    for block in range(N_TP):
        lower = block * width
        part = by_columns(later_hidden[:, lower:lower + width], down_weight[:, lower:lower + width]).astype(jnp.bfloat16)
        total = total + lax.optimization_barrier(part).astype(jnp.float32)
    later_out = total.astype(jnp.bfloat16)

    gate_e = jnp.dot(earlier_rows, gate_weight, preferred_element_type=jnp.float32)
    up_e = jnp.dot(earlier_rows, up_weight, preferred_element_type=jnp.float32)
    activation, slope = silu_parts(gate_e)
    hidden_e = (activation * up_e).astype(jnp.bfloat16)
    back_hidden = jnp.dot(cotangent, down_weight, preferred_element_type=jnp.float32)
    gate_back = (back_hidden * up_e * slope).astype(jnp.bfloat16)
    up_back = (back_hidden * activation).astype(jnp.bfloat16)
    total = jnp.zeros((earlier_rows.shape[0], D), jnp.float32)
    for block in range(N_TP):
        lower = block * width
        part = by_columns(gate_back[:, lower:lower + width], gate_weight[:, lower:lower + width])
        part = part + by_columns(up_back[:, lower:lower + width], up_weight[:, lower:lower + width])
        total = total + lax.optimization_barrier(part.astype(jnp.bfloat16)).astype(jnp.float32)
    input_grad = total.astype(jnp.bfloat16)
    gate_grad_new = gate_grad_sum + by_rows(earlier_rows, gate_back)
    up_grad_new = up_grad_sum + by_rows(earlier_rows, up_back)
    down_grad_new = down_grad_sum + by_rows(cotangent, hidden_e)
    return later_out, input_grad, gate_grad_new, up_grad_new, down_grad_new
```

```python
import functools

import jax
import jax.numpy as jnp
from jax import lax
from jax.experimental import pallas as pl
from jax.experimental.pallas import tpu as pltpu
from jax.sharding import PartitionSpec as P


F32 = jnp.float32
BF16 = jnp.bfloat16
RING = 4
BLOCKS = RING * RING
LANES = 128


def device(z, x, y, c):
    return ((z % RING) * RING + x % RING) * 2 * RING + (y % RING) * 2 + c


def pairs(move):
    cells = [(z, x, y, c) for z in range(RING) for x in range(RING) for y in range(RING) for c in range(2)]
    return [(device(*p), device(*move(*p))) for p in cells]


def shift(value, move):
    return lax.ppermute(value, ("fs", "tp"), pairs(move))


def inner(value, d):
    return shift(value, lambda z, x, y, c: (z, x + d, y, c) if c == 0 else (z + d, x, y, c))


def outer(value, d):
    return shift(value, lambda z, x, y, c: (z + d, x, y, c) if c == 0 else (z, x + d, y, c))


def along_y(value, d):
    return shift(value, lambda z, x, y, c: (z, x, y + d, c))


def swap(value):
    return shift(value, lambda z, x, y, c: (z, x, y, 1 - c))


def picked_kernel(index, *refs, groups):
    outs = refs[-len(groups) :]
    ins = refs[: -len(groups)]
    at = 0
    for out, count in zip(outs, groups):
        for b in range(BLOCKS):
            start = pl.multiple_of(index[b] * LANES, LANES)
            total = ins[at][:, pl.ds(start, LANES)].astype(F32)
            for k in range(1, count):
                total = total + ins[at + k][:, pl.ds(start, LANES)].astype(F32)
            out[:, b * LANES : (b + 1) * LANES] = total.astype(out.dtype)
        at += count


def picked(index, *groups):
    flat = [a for g in groups for a in g]
    return pl.pallas_call(
        functools.partial(picked_kernel, groups=tuple(len(g) for g in groups)),
        out_shape=[jax.ShapeDtypeStruct(g[0].shape, BF16) for g in groups],
        in_specs=[pl.BlockSpec(memory_space=pltpu.SMEM)]
        + [pl.BlockSpec(memory_space=pltpu.VMEM)] * len(flat),
        out_specs=[pl.BlockSpec(memory_space=pltpu.VMEM)] * len(groups),
        name="picked",
    )(index, *flat)


def turned(b):
    return (b % RING) * RING + b // RING


def joined_kernel(own, other, out):
    step = pl.program_id(0)

    @pl.when(step < RING)
    def _():
        out[...] = own[...]

    @pl.when(step >= RING)
    def _():
        for b in range(BLOCKS):
            s = turned(b)
            out[:, b * LANES : (b + 1) * LANES] = other[:, s * LANES : (s + 1) * LANES]


def joined(own, other, which=0):
    rows = 112
    width = own.shape[1]
    base = which * RING
    return pl.pallas_call(
        joined_kernel,
        grid=(2 * RING,),
        in_specs=[
            pl.BlockSpec((rows, width), lambda g: (base + jnp.minimum(g, RING - 1), 0)),
            pl.BlockSpec((rows, width), lambda g: (base + jnp.maximum(g - RING, 0), 0)),
        ],
        out_specs=pl.BlockSpec((rows, width), lambda g: (g, 0)),
        out_shape=jax.ShapeDtypeStruct((2 * RING * rows, width), BF16),
        name="joined",
    )(own, other)


def turn_add_kernel(own, other, out):
    for b in range(BLOCKS):
        s = turned(b)
        here = slice(b * LANES, (b + 1) * LANES)
        out[:, here] = (
            own[:, here].astype(F32) + other[:, s * LANES : (s + 1) * LANES].astype(F32)
        ).astype(BF16)


def turn_add(own, other):
    rows = 112
    width = own.shape[1]
    spec = pl.BlockSpec((rows, width), lambda g: (g, 0))
    return pl.pallas_call(
        turn_add_kernel,
        grid=(own.shape[0] // rows,),
        in_specs=[spec, spec],
        out_specs=spec,
        out_shape=jax.ShapeDtypeStruct(own.shape, BF16),
        name="turn_add",
    )(own, other)


def ring_gathered(value, move, halves):
    first = move(value, -1)
    last = move(value, 1)
    cut = halves
    far = jnp.concatenate([move(first[:cut], -1), move(last[cut:], 1)], axis=0)
    return value, first, far, last


def weights_gathered(value):
    near = jnp.concatenate(
        [value, inner(value, -1), inner(value, 2), inner(value, 1)], axis=1
    )
    return jnp.concatenate(ring_gathered(near, outer, value.shape[0] // 2), axis=1)


def ring_summed(parts, move, cut):
    far = parts(2).astype(BF16)
    top = move(far[:cut], 1)
    bottom = move(far[cut:], -1)
    first = parts(1)
    first = jnp.concatenate([first[:cut] + top.astype(F32), first[cut:]], axis=0).astype(BF16)
    last = parts(3)
    last = jnp.concatenate([last[:cut], last[cut:] + bottom.astype(F32)], axis=0).astype(BF16)
    return parts(0), move(first, 1), move(last, -1)


def grads_summed(left, right, total):
    width = RING * LANES

    def part(r):
        return jnp.dot(left, right[:, r * width : (r + 1) * width], preferred_element_type=F32)

    own, a, b = ring_summed(part, outer, left.shape[0] // 2)
    near = (own + a.astype(F32) + b.astype(F32)).astype(BF16)
    p = [near[:, r * LANES : (r + 1) * LANES] for r in range(RING)]
    return (
        total
        + p[0].astype(F32)
        + inner(p[1], 1).astype(F32)
        + inner(p[2], 2).astype(F32)
        + inner(p[3], -1).astype(F32)
    )


def outputs_summed(left, right, index):
    half = left.shape[1] // 2

    def product(cols):
        return lax.dot_general(
            left[:, cols], right, (((0,), (0,)), ((), ())), preferred_element_type=F32
        ).astype(BF16)

    other = swap(product(slice(half, None)))
    both = turn_add(product(slice(0, half)), other)
    rows = half // RING

    def part(r):
        return both[r * rows : (r + 1) * rows].astype(F32)

    own, a, b = ring_summed(part, along_y, rows // 2)
    return picked(index, (own.astype(BF16), a, b))[0]


def by_columns(left, right):
    return lax.dot_general(
        left, right, (((1,), (1,)), ((), ())), preferred_element_type=F32
    )


def silu_parts(gate):
    sigma = jax.nn.sigmoid(gate)
    return (gate * sigma, sigma * (1.0 + gate * (1.0 - sigma)))


def local(
    later_rows,
    earlier_rows,
    cotangent,
    gate_weight,
    up_weight,
    down_weight,
    gate_grad_sum,
    up_grad_sum,
    down_grad_sum,
):
    fs, core = lax.axis_index("fs"), lax.axis_index("tp") % 2
    z, x = fs // RING, fs % RING
    block = jnp.arange(BLOCKS, dtype=jnp.int32)
    major, minor = block // RING, block % RING
    to_relative = jnp.where(
        core == 0,
        (z + major) % RING * RING + (x + minor) % RING,
        (z + minor) % RING * RING + (x + major) % RING,
    )
    dz, dx = (major - z) % RING, (minor - x) % RING
    to_absolute = jnp.where(core == 0, dz * RING + dx, dx * RING + dz)

    earlier, slope_in, later = picked(
        to_relative, (earlier_rows,), (cotangent,), (later_rows,)
    )
    width = gate_weight.shape[1]

    gate_up = weights_gathered(jnp.concatenate([gate_weight.T, up_weight.T], axis=0))
    rows = earlier.shape[0]
    pieces = ring_gathered(jnp.concatenate([earlier, slope_in], axis=0), along_y, rows)
    own = jnp.concatenate([p[:rows] for p in pieces] + [p[rows:] for p in pieces], axis=0)
    other = swap(own)
    rows_all = joined(own, other, 0)
    back_all = joined(own, other, 1)

    down = weights_gathered(down_weight.T)

    own_later = jnp.concatenate(ring_gathered(later, along_y, rows // 2), axis=0)
    later_all = joined(own_later, swap(own_later))

    both = by_columns(gate_up, rows_all)
    gate_e, up_e = both[:width], both[width:]
    activation, act_slope = silu_parts(gate_e)
    hidden_e = (activation * up_e).astype(BF16)
    down_new = grads_summed(hidden_e, back_all, down_grad_sum.T)

    back_hidden = by_columns(down, back_all)
    gate_back = (back_hidden * up_e * act_slope).astype(BF16)
    up_back = (back_hidden * activation).astype(BF16)
    gate_up_back = jnp.concatenate([gate_back, up_back], axis=0)
    gate_up_new = grads_summed(
        gate_up_back, rows_all, jnp.concatenate([gate_grad_sum.T, up_grad_sum.T], axis=0)
    )
    input_grad = outputs_summed(gate_up_back, gate_up, to_absolute)

    both_l = by_columns(gate_up, later_all)
    later_hidden = (jax.nn.silu(both_l[:width]) * both_l[width:]).astype(BF16)
    later_out = outputs_summed(later_hidden, down, to_absolute)
    return (later_out, input_grad, gate_up_new[:width].T, gate_up_new[width:].T, down_new.T)


def solution(mesh):
    rows, weights = P(("fs", "tp"), None), P("fs", "tp")
    return jax.shard_map(
        local,
        mesh=mesh,
        in_specs=(rows,) * 3 + (weights,) * 6,
        out_specs=(rows, rows, weights, weights, weights),
        check_vma=False,
    )
```
